32 devices in a mesh: sp: 16 (over z, y, x), tp: 2 (over core).
Axes of the slice: x: 2, y: 2, z: 4, core: 2. Of those that a mesh axis runs over, the one named last changes fastest.
Arguments:
- queries: bfloat16 [4096, 1024], P('sp', 'tp'), may hold values from -12 to 12
- keys: bfloat16 [4096, 1024], P('sp', 'tp'), may hold values from -6 to 6
- values: bfloat16 [4096, 1024], P('sp', 'tp'), may hold values from -6 to 6
- w_out: bfloat16 [1024, 2048], P(None, 'tp'), may hold values from -0.375 to 0.375
Outputs:
- mixed: bfloat16 [4096, 2048], P('sp', 'tp')
The draws below stay inside these ranges and needn't reach their ends.
All inputs are finite; a program needn't handle non-finite values.
Results may differ from the reference program's by a relative error of at most 0.0056.
Values may be sent and summed in bfloat16 or wider, within the bound.
A program may use at most 64 MiB of HBM per device.

```python
import math
import jax
import jax.numpy as jnp
from jax import lax

HEADS = 8
HEAD_DIM = 128
D = 2048
SIDE_KEY_COUNT = 64
MIDDLE_DILATION = 4
FAR_DILATION = 16
TOKENS = 4096


def draw_queries(key, part):
    shape = (TOKENS, HEADS * HEAD_DIM)
    drawn = jnp.clip(2.0 * jax.random.normal(jax.random.fold_in(key, 1), shape, jnp.float32), -12.0, 12.0)
    return drawn.astype(jnp.bfloat16)


def draw_keys(key, part):
    shape = (TOKENS, HEADS * HEAD_DIM)
    drawn = jnp.clip(jax.random.normal(jax.random.fold_in(key, 2), shape, jnp.float32), -6.0, 6.0)
    return drawn.astype(jnp.bfloat16)


def levels(own_key, shape, split, least, largest):
    def one(dim, blocks):
        draws = jax.random.uniform(jax.random.fold_in(jax.random.fold_in(own_key, 6), dim), (blocks,), jnp.float32, least / len(split), largest / len(split))
        return jnp.repeat(jnp.exp(draws), shape[dim] // blocks).reshape((-1,) + (1,) * (len(shape) - dim - 1))

    loudness = one(*split[0])
    for cut in split[1:]:
        loudness = loudness * one(*cut)
    return loudness


def gaussian(own_key, shape, width, bound, cuts=(), kind=jnp.bfloat16):
    level = levels(own_key, shape, cuts, -0.22, 0.18) if cuts else 1.0
    values = jax.random.normal(own_key, shape, jnp.float32) * width * level
    return jnp.minimum(jnp.maximum(values, -bound), bound).astype(kind)


def setup_inputs(seed: int = 0) -> dict:
    key_of = jax.random.split(jax.random.key(seed), 5)
    queries = draw_queries(jax.random.fold_in(key_of[4], 71), 0)
    keys = draw_keys(jax.random.fold_in(key_of[4], 71), 0)
    values = gaussian(key_of[2], (TOKENS, HEADS * HEAD_DIM), 1.0, 6.0, ((0, 16), (1, 2)))
    w_out = gaussian(key_of[3], (HEADS * HEAD_DIM, D), (HEADS * HEAD_DIM // 4) ** -0.5, 0.375, ((1, 2),))
    return dict(queries=queries, keys=keys, values=values, w_out=w_out)


def block_rows(count):
    return count if count <= 128 else math.gcd(count, 128)


def band_scores(queries, keys, values, dilation_step):
    sequence_length, columns = queries.shape
    heads = columns // HEAD_DIM
    residue_rows = sequence_length // dilation_step
    rows_block = block_rows(residue_rows)
    blocks = residue_rows // rows_block
    span = rows_block + 2 * SIDE_KEY_COUNT
    padding = SIDE_KEY_COUNT * dilation_step
    padded_keys = jnp.pad(keys, ((padding, padding), (0, 0))).reshape(residue_rows + 2 * SIDE_KEY_COUNT, dilation_step, heads, HEAD_DIM)
    padded_values = jnp.pad(values, ((padding, padding), (0, 0))).reshape(residue_rows + 2 * SIDE_KEY_COUNT, dilation_step, heads, HEAD_DIM)
    grouped = queries.reshape(blocks, rows_block, dilation_step, heads, HEAD_DIM)
    query_idx = jnp.arange(rows_block, dtype=jnp.int32)[:, None]
    key_idx = jnp.arange(span, dtype=jnp.int32)[None, :]
    in_band = (key_idx >= query_idx) & (key_idx <= query_idx + 2 * SIDE_KEY_COUNT)
    residues = jnp.arange(dilation_step, dtype=jnp.int32)[:, None, None, None]
    scale = HEAD_DIM ** -0.5

    def one_block(inputs):
        number, query_block = inputs
        first_row = (number * rows_block).astype(jnp.int32)
        key_window = lax.dynamic_slice_in_dim(padded_keys, first_row, span, 0)
        value_window = lax.dynamic_slice_in_dim(padded_values, first_row, span, 0)
        scores = jnp.einsum('qrhe,krhe->rhqk', query_block.astype(jnp.float32), key_window.astype(jnp.float32)) * scale
        key_pos = (first_row + key_idx[None, None] - SIDE_KEY_COUNT) * dilation_step + residues
        allowed = in_band[None, None] & (key_pos >= 0) & (key_pos < sequence_length)
        scores = jnp.where(allowed, scores, -jnp.inf)
        maximum = jnp.max(scores, axis=-1, keepdims=True)
        raised = jnp.exp(scores - maximum)
        denominator = jnp.sum(raised, axis=-1, keepdims=True)
        weights = (raised / denominator).astype(jnp.bfloat16)
        attended = jnp.einsum('rhqk,krhe->qrhe', weights.astype(jnp.float32), value_window.astype(jnp.float32))
        log_den = (maximum + jnp.log(denominator))[..., 0]
        return attended, jnp.transpose(log_den, (2, 0, 1))

    outputs, log_dens = lax.map(one_block, (jnp.arange(blocks, dtype=jnp.int32), grouped))
    return outputs.reshape(sequence_length, heads, HEAD_DIM), log_dens.reshape(sequence_length, heads)


def reference(queries, keys, values, w_out):
    sequence_length, columns = queries.shape
    group_results = [band_scores(queries, keys, values, dilation_step) for dilation_step in (1, MIDDLE_DILATION, FAR_DILATION)]
    stacked_out = jnp.stack([item[0] for item in group_results])
    stacked_den = jnp.stack([item[1] for item in group_results])
    shares = jax.nn.softmax(stacked_den, axis=0)
    attended = jnp.sum(shares[..., None] * stacked_out, axis=0).astype(jnp.bfloat16).reshape(sequence_length, columns)
    return jnp.dot(attended, w_out, preferred_element_type=jnp.float32).astype(jnp.bfloat16)
```

```python
import functools
import math

import jax
import jax.numpy as jnp
from jax import lax
from jax.experimental import pallas as pl
from jax.experimental.pallas import tpu as pltpu
from jax.sharding import PartitionSpec as P

HEAD_DIM = 128
SIDE = 64
MID = 4
FAR = 16
MESH = pl.DeviceIdType.MESH
F32 = jnp.float32
BF16 = jnp.bfloat16
SCALE = HEAD_DIM ** -0.5 * math.log2(math.e)


def nt(a, b):
    return lax.dot_general(a, b, (((1,), (1,)), ((), ())), preferred_element_type=F32)


def nn(a, b):
    return lax.dot_general(a, b, (((1,), (0,)), ((), ())), preferred_element_type=F32)


def iota(shape, dim):
    return lax.broadcasted_iota(jnp.int32, shape, dim)


def attend(q, k, v, allowed):
    s = jnp.where(allowed, nt(q, k) * SCALE, -jnp.inf)
    top = jnp.max(s, axis=-1, keepdims=True)
    raised = jnp.exp2(s - top)
    den = jnp.sum(raised, axis=-1, keepdims=True)
    return nn(raised.astype(BF16), v), top, den


def kernel(sp_n, heads, q_hbm, k_hbm, v_hbm, w_hbm, out_ref,
           q_in, k_in, v_in, w, pq, pkv, qf, kvf, near_lo, near_hi, ob, ret, att, att_other, acc_n, md_n,
           load_sem, kv_s, kv_r, q_s, q_r, up_s, up_r, dn_s, dn_r, near_s, near_r, ret_s, ret_r, tp_s, tp_r):
    rows = q_in.shape[0]
    chunk = rows // MID
    mm = rows // FAR
    e = HEAD_DIM
    p, c = lax.axis_index("sp"), lax.axis_index("tp")
    groups = sp_n // MID
    g, j = p // MID, p % MID

    loads = [
        pltpu.make_async_copy(src, dst, load_sem.at[n])
        for n, (src, dst) in enumerate(((k_hbm, k_in), (v_hbm, v_in), (q_hbm, q_in), (w_hbm, w)))
    ]
    for load in loads:
        load.start()

    barrier = pltpu.get_barrier_semaphore()

    def greet(sp, tp):
        pl.semaphore_signal(barrier, inc=1, device_id=(sp, tp), device_id_type=MESH)

    def mate(d):
        return g * MID + (j + d) % MID

    for d in range(1, MID):
        greet(mate(d), c)
    greet(p, 1 - c)
    has_dn, has_up = g > 0, g < groups - 1
    has_prev, has_next = p > 0, p < sp_n - 1

    @pl.when(has_dn)
    def _():
        greet(p - MID, c)

    @pl.when(has_up)
    def _():
        greet(p + MID, c)

    @pl.when(has_prev)
    def _():
        greet(p - 1, c)

    @pl.when(has_next)
    def _():
        greet(p + 1, c)

    def remote(src, dst, ss, rs, sp, tp):
        return pltpu.make_async_remote_copy(
            src_ref=src, dst_ref=dst, send_sem=ss, recv_sem=rs, device_id=(sp, tp), device_id_type=MESH)

    r, t = iota((rows, rows), 0), iota((rows, rows), 1)
    perm = (t == FAR * (r % mm) + MID * ((r % chunk) // mm) + r // chunk).astype(BF16)
    r, t = t, r
    back = (t == FAR * (r % mm) + MID * ((r % chunk) // mm) + r // chunk).astype(BF16)

    loads[0].wait()
    loads[1].wait()
    pk = nn(perm, k_in[...]).astype(BF16)
    pv = nn(perm, v_in[...]).astype(BF16)
    for h in range(heads):
        pkv[h, 0] = pk[:, h * e:(h + 1) * e]
        pkv[h, 1] = pv[:, h * e:(h + 1) * e]

    def at(n, base=0):
        return pl.ds(pl.multiple_of(base + n * chunk, chunk), chunk)

    for h in range(heads):
        for n in range(2):
            kvf[h, n, at(j, rows), :] = pkv[h, n, at(j), :]

    def edge(test, rows_at, near):
        @pl.when(jnp.logical_not(test))
        def _():
            for h in range(heads):
                for n in range(2):
                    kvf[h, n, pl.ds(rows_at, rows), :] = jnp.zeros((rows, e), BF16)

    edge(has_dn, 0, near_lo)
    edge(has_up, 2 * rows, near_hi)

    @pl.when(jnp.logical_not(has_prev))
    def _():
        near_lo[...] = jnp.zeros_like(near_lo)

    @pl.when(jnp.logical_not(has_next))
    def _():
        near_hi[...] = jnp.zeros_like(near_hi)

    pl.semaphore_wait(
        barrier,
        MID + has_dn.astype(jnp.int32) + has_up.astype(jnp.int32)
        + has_prev.astype(jnp.int32) + has_next.astype(jnp.int32))

    def up(h, d):
        n = (j - d + MID) % MID
        src = pkv.at[h, :, at(n), :] if d == 0 else kvf.at[h, :, at(n, rows), :]
        return remote(src, kvf.at[h, :, at(n), :], up_s.at[h, d], up_r.at[h, d], (p + MID) % sp_n, c)

    def down(h, d):
        n = (j - d + MID) % MID
        src = pkv.at[h, :, at(n), :] if d == 0 else kvf.at[h, :, at(n, rows), :]
        return remote(src, kvf.at[h, :, at(n, 2 * rows), :], dn_s.at[h, d], dn_r.at[h, d], (p - MID + sp_n) % sp_n, c)

    def forward(h, d):
        @pl.when(has_up)
        def _():
            up(h, d).start()

        @pl.when(has_dn)
        def _():
            down(h, d).start()

    def kv(h, d, receive=False):
        dst = (j - d + MID) % MID if receive else j
        return remote(pkv.at[h, :, at((j + d) % MID), :], kvf.at[h, :, at(dst, rows), :],
                      kv_s.at[h, d - 1], kv_r.at[h, d - 1], mate(d), c)

    def queries(d, receive=False):
        dst = (j - d + MID) % MID if receive else j
        return remote(pq.at[:, at((j + d) % MID), :], qf.at[:, at(dst), :],
                      q_s.at[d - 1], q_r.at[d - 1], mate(d), c)

    for h in range(heads):
        for d in range(1, MID):
            kv(h, d).start()
        forward(h, 0)

    loads[2].wait()
    pq_all = nn(perm, q_in[...]).astype(BF16)
    for h in range(heads):
        pq[h] = pq_all[:, h * e:(h + 1) * e]
    for h in range(heads):
        qf[h, at(j), :] = pq[h, at(j), :]
    for d in range(1, MID):
        queries(d).start()

    def near(n, to_next):
        src = (k_in, v_in)[n]
        if to_next:
            return remote(src.at[pl.ds(rows - SIDE, SIDE), :], near_lo.at[n],
                          near_s.at[n, 0], near_r.at[n, 0], (p + 1) % sp_n, c)
        return remote(src.at[pl.ds(0, SIDE), :], near_hi.at[n],
                      near_s.at[n, 1], near_r.at[n, 1], (p - 1 + sp_n) % sp_n, c)

    @pl.when(has_next)
    def _():
        for n in range(2):
            near(n, True).start()

    @pl.when(has_prev)
    def _():
        for n in range(2):
            near(n, False).start()

    for h in range(heads):
        for d in range(1, MID):
            kv(h, d, receive=True).wait_recv()
            forward(h, d)

    @pl.when(has_prev)
    def _():
        for n in range(2):
            near(n, True).wait_recv()

    @pl.when(has_next)
    def _():
        for n in range(2):
            near(n, False).wait_recv()

    half = rows // 2
    span = half + 2 * SIDE
    qi, ki = iota((half, span), 0), iota((half, span), 1)
    band = (ki >= qi) & (ki <= qi + 2 * SIDE)
    lo_ok, hi_ok = has_prev.astype(jnp.int32), has_next.astype(jnp.int32)
    allowed = (band & ((ki >= SIDE) | (lo_ok == 1)), band & ((ki < span - SIDE) | (hi_ok == 1)))
    for h in range(heads):
        cols = slice(h * e, (h + 1) * e)
        ks = [jnp.concatenate([near_lo[n, :, cols], x[:, cols], near_hi[n, :, cols]], axis=0)
              for n, x in enumerate((k_in, v_in))]
        for b in range(2):
            at_b = slice(b * half, (b + 1) * half)
            o, top, den = attend(q_in[at_b, cols], ks[0][b * half:b * half + span],
                                 ks[1][b * half:b * half + span], allowed[b])
            acc_n[h, at_b, :] = o
            md_n[h, 0, at_b, :] = jnp.broadcast_to(top, (half, e))
            md_n[h, 1, at_b, :] = jnp.broadcast_to(den, (half, e))

    for d in range(1, MID):
        queries(d, receive=True).wait_recv()

    def order(x):
        return chunk * (x // chunk) + (FAR // MID) * (x % mm) + (x % chunk) // mm

    dn_ok, up_ok = has_dn.astype(jnp.int32), has_up.astype(jnp.int32)
    gap = order(ki) - order(qi)
    band = (gap >= 0) & (gap <= 2 * SIDE)
    mid_ok = (band & ((ki >= SIDE) | (dn_ok == 1)), band & ((ki < span - SIDE) | (up_ok == 1)))
    far_span = 3 * chunk
    qi, ki = iota((chunk, far_span), 0), iota((chunk, far_span), 1)
    far_ok = ((ki >= qi) & (ki <= qi + 2 * SIDE) & ((ki >= chunk) | (dn_ok == 1))
              & ((ki < 2 * chunk) | (up_ok == 1)))
    lane = iota((rows, e), 1)

    def result(h, d, receive=False):
        dst = (j - d + MID) % MID if receive else j
        return remote(ob.at[h, :, at((j + d) % MID), :], ret.at[h, :, at(dst), :],
                      ret_s.at[h, d - 1], ret_r.at[h, d - 1], mate(d), c)

    for h in range(heads):
        @pl.when(has_dn)
        def _():
            for d in range(MID):
                up(h, d).wait_recv()

        @pl.when(has_up)
        def _():
            for d in range(MID):
                down(h, d).wait_recv()

        q = qf[h]
        kh, vh = kvf[h, 0], kvf[h, 1]
        mids = []
        for b in range(2):
            first = rows - chunk + b * half
            mids.append(attend(q[b * half:(b + 1) * half], kh[first:first + span], vh[first:first + span], mid_ok[b]))
        o1, t1, d1 = (jnp.concatenate([mids[0][n], mids[1][n]], axis=0) for n in range(3))
        q4 = q.reshape(MID, FAR // MID, mm, e)
        k4 = kh.reshape(3 * MID, FAR // MID, mm, e)
        v4 = vh.reshape(3 * MID, FAR // MID, mm, e)
        fars = [
            attend(q4[:, s].reshape(chunk, e), k4[:, s].reshape(far_span, e), v4[:, s].reshape(far_span, e), far_ok)
            for s in range(FAR // MID)
        ]
        o2, t2, d2 = (
            jnp.concatenate(
                [fars[s][n][i * mm:(i + 1) * mm] for i in range(MID) for s in range(FAR // MID)], axis=0)
            for n in range(3))
        top = jnp.maximum(t1, t2)
        e1, e2 = jnp.exp2(t1 - top), jnp.exp2(t2 - top)
        den = e1 * d1 + e2 * d2
        ob[h, 0] = ((e1 * o1 + e2 * o2) / den).astype(BF16)
        log_den = jnp.broadcast_to(top + jnp.log2(den), (rows, e))
        one = log_den.astype(BF16).astype(F32)
        two = (log_den - one).astype(BF16).astype(F32)
        three = log_den - one - two
        ob[h, 1] = jnp.where(lane == 0, one, jnp.where(lane == 1, two, three)).astype(BF16)
        for d in range(1, MID):
            result(h, d).start()
        for n in range(2):
            ret[h, n, at(j), :] = ob[h, n, at(j), :]

    def share(h):
        cols = pl.ds(h * e, e)
        return remote(att.at[:, cols], att_other.at[:, cols], tp_s.at[h], tp_r.at[h], p, 1 - c)

    for h in range(heads):
        for d in range(1, MID):
            result(h, d, receive=True).wait_recv()
        both = nn(back, jnp.concatenate([ret[h, 0], ret[h, 1]], axis=1))
        o, parts = both[:, :e], both[:, e:]
        log_den = parts[:, 0:1] + parts[:, 1:2] + parts[:, 2:3]
        t_n, d_n = md_n[h, 0], md_n[h, 1]
        top = jnp.maximum(t_n, log_den)
        e1, e2 = jnp.exp2(t_n - top), jnp.exp2(log_den - top)
        att[:, h * e:(h + 1) * e] = ((e1 * acc_n[h] + e2 * o) / (e1 * d_n + e2)).astype(BF16)
        share(h).start()

    width = heads * e
    loads[3].wait()
    own = nn(att[...], w[pl.ds(pl.multiple_of(c * width, width), width), :])
    for h in range(heads):
        share(h).wait_recv()
    other = nn(att_other[...], w[pl.ds(pl.multiple_of((1 - c) * width, width), width), :])
    out_ref[...] = (own + other).astype(BF16)

    for h in range(heads):
        for d in range(1, MID):
            kv(h, d).wait_send()
            result(h, d).wait_send()
        share(h).wait_send()
    for d in range(1, MID):
        queries(d).wait_send()

    @pl.when(has_up)
    def _():
        for h in range(heads):
            for d in range(MID):
                up(h, d).wait_send()

    @pl.when(has_dn)
    def _():
        for h in range(heads):
            for d in range(MID):
                down(h, d).wait_send()

    @pl.when(has_next)
    def _():
        for n in range(2):
            near(n, True).wait_send()

    @pl.when(has_prev)
    def _():
        for n in range(2):
            near(n, False).wait_send()


def per_device(sp_n, q, k, v, w):
    rows, columns = q.shape
    heads = columns // HEAD_DIM
    assert MID * rows == SIDE * FAR and rows // MID == SIDE and sp_n % MID == 0
    dma = pltpu.SemaphoreType.DMA
    e = HEAD_DIM
    return pl.pallas_call(
        functools.partial(kernel, sp_n, heads),
        out_shape=jax.ShapeDtypeStruct((rows, w.shape[1]), BF16),
        in_specs=[pl.BlockSpec(memory_space=pl.ANY)] * 4,
        out_specs=pl.BlockSpec(memory_space=pltpu.VMEM),
        scratch_shapes=[
            pltpu.VMEM((rows, columns), BF16),
            pltpu.VMEM((rows, columns), BF16),
            pltpu.VMEM((rows, columns), BF16),
            pltpu.VMEM(w.shape, BF16),
            pltpu.VMEM((heads, rows, e), BF16),
            pltpu.VMEM((heads, 2, rows, e), BF16),
            pltpu.VMEM((heads, rows, e), BF16),
            pltpu.VMEM((heads, 2, 3 * rows, e), BF16),
            pltpu.VMEM((2, SIDE, columns), BF16),
            pltpu.VMEM((2, SIDE, columns), BF16),
            pltpu.VMEM((heads, 2, rows, e), BF16),
            pltpu.VMEM((heads, 2, rows, e), BF16),
            pltpu.VMEM((rows, columns), BF16),
            pltpu.VMEM((rows, columns), BF16),
            pltpu.VMEM((heads, rows, e), F32),
            pltpu.VMEM((heads, 2, rows, e), F32),
            dma((4,)),
            dma((heads, MID - 1)), dma((heads, MID - 1)),
            dma((MID - 1,)), dma((MID - 1,)),
            dma((heads, MID)), dma((heads, MID)),
            dma((heads, MID)), dma((heads, MID)),
            dma((2, 2)), dma((2, 2)),
            dma((heads, MID - 1)), dma((heads, MID - 1)),
            dma((heads,)), dma((heads,)),
        ],
        compiler_params=pltpu.CompilerParams(collective_id=0, has_side_effects=True),
    )(q, k, v, w)


def solution(mesh):
    return jax.shard_map(
        functools.partial(per_device, mesh.shape["sp"]), mesh=mesh,
        in_specs=(P("sp", "tp"), P("sp", "tp"), P("sp", "tp"), P(None, "tp")),
        out_specs=P("sp", "tp"), check_vma=False,
    )
```

```python
import functools
import math

import jax
import jax.numpy as jnp
from jax import lax
from jax.experimental import pallas as pl
from jax.experimental.pallas import tpu as pltpu
from jax.sharding import PartitionSpec as P

HEAD_DIM = 128
SIDE = 64
MID = 4
FAR = 16
MESH = pl.DeviceIdType.MESH
F32 = jnp.float32
BF16 = jnp.bfloat16
SCALE = HEAD_DIM ** -0.5 * math.log2(math.e)


def nt(a, b):
    return lax.dot_general(a, b, (((1,), (1,)), ((), ())), preferred_element_type=F32)


def nn(a, b):
    return lax.dot_general(a, b, (((1,), (0,)), ((), ())), preferred_element_type=F32)


def iota(shape, dim):
    return lax.broadcasted_iota(jnp.int32, shape, dim)


def attend(q, k, v, allowed):
    s = jnp.where(allowed, nt(q, k) * SCALE, -jnp.inf)
    top = jnp.max(s, axis=-1, keepdims=True)
    raised = jnp.exp2(s - top)
    den = jnp.sum(raised, axis=-1, keepdims=True)
    return nn(raised.astype(BF16), v), top, den


def kernel(sp_n, heads, q_hbm, k_hbm, v_hbm, w_hbm, out_ref,
           q_in, k_in, v_in, w, pkv, kvf, near_lo, near_hi, ob, ret, att, att_other, acc_n, md_n,
           load_sem, kv_s, kv_r, up_s, up_r, dn_s, dn_r, near_s, near_r, ret_s, ret_r, tp_s, tp_r):
    rows = q_in.shape[0]
    chunk = rows // MID
    mm = rows // FAR
    e = HEAD_DIM
    p, c = lax.axis_index("sp"), lax.axis_index("tp")
    groups = sp_n // MID
    g, j = p // MID, p % MID

    loads = [
        pltpu.make_async_copy(src, dst, load_sem.at[n])
        for n, (src, dst) in enumerate(((k_hbm, k_in), (v_hbm, v_in), (q_hbm, q_in), (w_hbm, w)))
    ]
    for load in loads:
        load.start()

    barrier = pltpu.get_barrier_semaphore()

    def greet(sp, tp):
        pl.semaphore_signal(barrier, inc=1, device_id=(sp, tp), device_id_type=MESH)

    def mate(d):
        return g * MID + (j + d) % MID

    for d in range(1, MID):
        greet(mate(d), c)
    greet(p, 1 - c)
    has_dn, has_up = g > 0, g < groups - 1
    has_prev, has_next = p > 0, p < sp_n - 1

    @pl.when(has_dn)
    def _():
        greet(p - MID, c)

    @pl.when(has_up)
    def _():
        greet(p + MID, c)

    @pl.when(has_prev)
    def _():
        greet(p - 1, c)

    @pl.when(has_next)
    def _():
        greet(p + 1, c)

    def remote(src, dst, ss, rs, sp, tp):
        return pltpu.make_async_remote_copy(
            src_ref=src, dst_ref=dst, send_sem=ss, recv_sem=rs, device_id=(sp, tp), device_id_type=MESH)

    r, t = iota((rows, rows), 0), iota((rows, rows), 1)
    perm = (t == FAR * (r % mm) + MID * ((r % chunk) // mm) + r // chunk).astype(BF16)
    r, t = t, r
    back = (t == FAR * (r % mm) + MID * ((r % chunk) // mm) + r // chunk).astype(BF16)

    for n, x in enumerate((k_in, v_in, q_in)):
        loads[n].wait()
        moved = nn(perm, x[...]).astype(BF16)
        for h in range(heads):
            pkv[h, n] = moved[:, h * e:(h + 1) * e]

    def at(n, base=0):
        return pl.ds(pl.multiple_of(base + n * chunk, chunk), chunk)

    for h in range(heads):
        for n in range(3):
            kvf[h, n, at(j, rows), :] = pkv[h, n, at(j), :]

    def edge(test, rows_at):
        @pl.when(jnp.logical_not(test))
        def _():
            for h in range(heads):
                for n in range(2):
                    kvf[h, n, pl.ds(rows_at, rows), :] = jnp.zeros((rows, e), BF16)

    edge(has_dn, 0)
    edge(has_up, 2 * rows)

    @pl.when(jnp.logical_not(has_prev))
    def _():
        near_lo[...] = jnp.zeros_like(near_lo)

    @pl.when(jnp.logical_not(has_next))
    def _():
        near_hi[...] = jnp.zeros_like(near_hi)

    pl.semaphore_wait(
        barrier,
        MID + has_dn.astype(jnp.int32) + has_up.astype(jnp.int32)
        + has_prev.astype(jnp.int32) + has_next.astype(jnp.int32))

    def up(h, d):
        n = (j - d + MID) % MID
        src = pkv.at[h, 0:2, at(n), :] if d == 0 else kvf.at[h, 0:2, at(n, rows), :]
        return remote(src, kvf.at[h, 0:2, at(n), :], up_s.at[h, d], up_r.at[h, d], (p + MID) % sp_n, c)

    def down(h, d):
        n = (j - d + MID) % MID
        src = pkv.at[h, 0:2, at(n), :] if d == 0 else kvf.at[h, 0:2, at(n, rows), :]
        return remote(src, kvf.at[h, 0:2, at(n, 2 * rows), :], dn_s.at[h, d], dn_r.at[h, d], (p - MID + sp_n) % sp_n, c)

    def forward(h, d):
        @pl.when(has_up)
        def _():
            up(h, d).start()

        @pl.when(has_dn)
        def _():
            down(h, d).start()

    def kv(h, d, receive=False):
        dst = (j - d + MID) % MID if receive else j
        return remote(pkv.at[h, :, at((j + d) % MID), :], kvf.at[h, :, at(dst, rows), :],
                      kv_s.at[h, d - 1], kv_r.at[h, d - 1], mate(d), c)

    for h in range(heads):
        for d in range(1, MID):
            kv(h, d).start()
        forward(h, 0)

    def near(n, to_next):
        src = (k_in, v_in)[n]
        if to_next:
            return remote(src.at[pl.ds(rows - SIDE, SIDE), :], near_lo.at[n],
                          near_s.at[n, 0], near_r.at[n, 0], (p + 1) % sp_n, c)
        return remote(src.at[pl.ds(0, SIDE), :], near_hi.at[n],
                      near_s.at[n, 1], near_r.at[n, 1], (p - 1 + sp_n) % sp_n, c)

    @pl.when(has_next)
    def _():
        for n in range(2):
            near(n, True).start()

    @pl.when(has_prev)
    def _():
        for n in range(2):
            near(n, False).start()

    for h in range(heads):
        for d in range(1, MID):
            kv(h, d, receive=True).wait_recv()
            forward(h, d)

    half = rows // 2
    span = half + 2 * SIDE
    qi, ki = iota((half, span), 0), iota((half, span), 1)

    def order(x):
        return chunk * (x // chunk) + (FAR // MID) * (x % mm) + (x % chunk) // mm

    dn_ok, up_ok = has_dn.astype(jnp.int32), has_up.astype(jnp.int32)
    gap = order(ki) - order(qi)
    band = (gap >= 0) & (gap <= 2 * SIDE)
    mid_ok = (band & ((ki >= SIDE) | (dn_ok == 1)), band & ((ki < span - SIDE) | (up_ok == 1)))
    far_span = 3 * chunk
    qi, ki = iota((chunk, far_span), 0), iota((chunk, far_span), 1)
    far_ok = ((ki >= qi) & (ki <= qi + 2 * SIDE) & ((ki >= chunk) | (dn_ok == 1))
              & ((ki < 2 * chunk) | (up_ok == 1)))
    lane = iota((rows, e), 1)
    pick = (iota((16, e), 0) == iota((16, e), 1)).astype(BF16)

    def result(h, d, receive=False):
        dst = (j - d + MID) % MID if receive else j
        return remote(ob.at[h, (j + d) % MID], ret.at[h, dst],
                      ret_s.at[h, d - 1], ret_r.at[h, d - 1], mate(d), c)

    for h in range(heads):
        @pl.when(has_dn)
        def _():
            for d in range(MID):
                up(h, d).wait_recv()

        @pl.when(has_up)
        def _():
            for d in range(MID):
                down(h, d).wait_recv()

        q = kvf[h, 2, pl.ds(rows, rows), :]
        kh, vh = kvf[h, 0], kvf[h, 1]
        mids = []
        for b in range(2):
            first = rows - chunk + b * half
            mids.append(attend(q[b * half:(b + 1) * half], kh[first:first + span], vh[first:first + span], mid_ok[b]))
        o1, t1, d1 = (jnp.concatenate([mids[0][n], mids[1][n]], axis=0) for n in range(3))
        q4 = q.reshape(MID, FAR // MID, mm, e)
        k4 = kh.reshape(3 * MID, FAR // MID, mm, e)
        v4 = vh.reshape(3 * MID, FAR // MID, mm, e)
        fars = [
            attend(q4[:, s].reshape(chunk, e), k4[:, s].reshape(far_span, e), v4[:, s].reshape(far_span, e), far_ok)
            for s in range(FAR // MID)
        ]
        o2, t2, d2 = (
            jnp.concatenate(
                [fars[s][n][i * mm:(i + 1) * mm] for i in range(MID) for s in range(FAR // MID)], axis=0)
            for n in range(3))
        top = jnp.maximum(t1, t2)
        e1, e2 = jnp.exp2(t1 - top), jnp.exp2(t2 - top)
        den = e1 * d1 + e2 * d2
        o = ((e1 * o1 + e2 * o2) / den).astype(BF16)
        log_den = jnp.broadcast_to(top + jnp.log2(den), (rows, e))
        one = log_den.astype(BF16).astype(F32)
        two = (log_den - one).astype(BF16).astype(F32)
        three = log_den - one - two
        parts = jnp.where(lane == 0, one, jnp.where(lane == 1, two, three)).astype(BF16)
        twice = [parts[i * chunk:(i + 1) * chunk] for i in range(MID) for _ in range(2)]
        flat = nt(pick, jnp.concatenate(twice, axis=0)).astype(BF16)
        for i in range(MID):
            ob[h, i, :chunk] = o[i * chunk:(i + 1) * chunk]
            ob[h, i, chunk:] = flat[:, 2 * i * chunk:2 * (i + 1) * chunk]
        for d in range(1, MID):
            result(h, d).start()
        ret[h, pl.ds(j, 1)] = ob[h, pl.ds(j, 1)]

    @pl.when(has_prev)
    def _():
        for n in range(2):
            near(n, True).wait_recv()

    @pl.when(has_next)
    def _():
        for n in range(2):
            near(n, False).wait_recv()

    qi, ki = iota((half, span), 0), iota((half, span), 1)
    band = (ki >= qi) & (ki <= qi + 2 * SIDE)
    lo_ok, hi_ok = has_prev.astype(jnp.int32), has_next.astype(jnp.int32)
    allowed = (band & ((ki >= SIDE) | (lo_ok == 1)), band & ((ki < span - SIDE) | (hi_ok == 1)))
    for h in range(heads):
        cols = slice(h * e, (h + 1) * e)
        ks = [jnp.concatenate([near_lo[n, :, cols], x[:, cols], near_hi[n, :, cols]], axis=0)
              for n, x in enumerate((k_in, v_in))]
        for b in range(2):
            at_b = slice(b * half, (b + 1) * half)
            o, top, den = attend(q_in[at_b, cols], ks[0][b * half:b * half + span],
                                 ks[1][b * half:b * half + span], allowed[b])
            acc_n[h, at_b, :] = o
            md_n[h, 0, at_b, :] = jnp.broadcast_to(top, (half, e))
            md_n[h, 1, at_b, :] = jnp.broadcast_to(den, (half, e))

    r, t = iota((rows, 2 * rows), 1), iota((rows, 2 * rows), 0)
    low = r % (2 * chunk) < chunk
    r = r // (2 * chunk) * chunk + r % (2 * chunk)
    back_twice = (low & (t == FAR * (r % mm) + MID * ((r % chunk) // mm) + r // chunk)).astype(BF16)

    def share(h):
        cols = pl.ds(h * e, e)
        return remote(att.at[:, cols], att_other.at[:, cols], tp_s.at[h], tp_r.at[h], p, 1 - c)

    for h in range(heads):
        for d in range(1, MID):
            result(h, d, receive=True).wait_recv()
        o = nn(back, jnp.concatenate([ret[h, i, :chunk] for i in range(MID)], axis=0))
        parts = nt(back_twice, jnp.concatenate([ret[h, i, chunk:] for i in range(MID)], axis=1))
        log_den = parts[:, 0:1] + parts[:, 1:2] + parts[:, 2:3]
        t_n, d_n = md_n[h, 0], md_n[h, 1]
        top = jnp.maximum(t_n, log_den)
        e1, e2 = jnp.exp2(t_n - top), jnp.exp2(log_den - top)
        att[:, h * e:(h + 1) * e] = ((e1 * acc_n[h] + e2 * o) / (e1 * d_n + e2)).astype(BF16)
        share(h).start()

    width = heads * e
    loads[3].wait()
    own = nn(att[...], w[pl.ds(pl.multiple_of(c * width, width), width), :])
    for h in range(heads):
        share(h).wait_recv()
    other = nn(att_other[...], w[pl.ds(pl.multiple_of((1 - c) * width, width), width), :])
    out_ref[...] = (own + other).astype(BF16)

    for h in range(heads):
        for d in range(1, MID):
            kv(h, d).wait_send()
            result(h, d).wait_send()
        share(h).wait_send()
    @pl.when(has_up)
    def _():
        for h in range(heads):
            for d in range(MID):
                up(h, d).wait_send()

    @pl.when(has_dn)
    def _():
        for h in range(heads):
            for d in range(MID):
                down(h, d).wait_send()

    @pl.when(has_next)
    def _():
        for n in range(2):
            near(n, True).wait_send()

    @pl.when(has_prev)
    def _():
        for n in range(2):
            near(n, False).wait_send()


def per_device(sp_n, q, k, v, w):
    rows, columns = q.shape
    heads = columns // HEAD_DIM
    assert MID * rows == SIDE * FAR and rows // MID == SIDE and sp_n % MID == 0
    dma = pltpu.SemaphoreType.DMA
    e, chunk = HEAD_DIM, rows // MID
    return pl.pallas_call(
        functools.partial(kernel, sp_n, heads),
        out_shape=jax.ShapeDtypeStruct((rows, w.shape[1]), BF16),
        in_specs=[pl.BlockSpec(memory_space=pl.ANY)] * 4,
        out_specs=pl.BlockSpec(memory_space=pltpu.VMEM),
        scratch_shapes=[
            pltpu.VMEM((rows, columns), BF16),
            pltpu.VMEM((rows, columns), BF16),
            pltpu.VMEM((rows, columns), BF16),
            pltpu.VMEM(w.shape, BF16),
            pltpu.VMEM((heads, 3, rows, e), BF16),
            pltpu.VMEM((heads, 3, 3 * rows, e), BF16),
            pltpu.VMEM((2, SIDE, columns), BF16),
            pltpu.VMEM((2, SIDE, columns), BF16),
            pltpu.VMEM((heads, MID, chunk + 16, e), BF16),
            pltpu.VMEM((heads, MID, chunk + 16, e), BF16),
            pltpu.VMEM((rows, columns), BF16),
            pltpu.VMEM((rows, columns), BF16),
            pltpu.VMEM((heads, rows, e), F32),
            pltpu.VMEM((heads, 2, rows, e), F32),
            dma((4,)),
            dma((heads, MID - 1)), dma((heads, MID - 1)),
            dma((heads, MID)), dma((heads, MID)),
            dma((heads, MID)), dma((heads, MID)),
            dma((2, 2)), dma((2, 2)),
            dma((heads, MID - 1)), dma((heads, MID - 1)),
            dma((heads,)), dma((heads,)),
        ],
        compiler_params=pltpu.CompilerParams(collective_id=0, has_side_effects=True),
    )(q, k, v, w)


def solution(mesh):
    return jax.shard_map(
        functools.partial(per_device, mesh.shape["sp"]), mesh=mesh,
        in_specs=(P("sp", "tp"), P("sp", "tp"), P("sp", "tp"), P(None, "tp")),
        out_specs=P("sp", "tp"), check_vma=False,
    )
```

```python
import functools
import math

import jax
import jax.numpy as jnp
from jax import lax
from jax.experimental import pallas as pl
from jax.experimental.pallas import tpu as pltpu
from jax.sharding import PartitionSpec as P

HEAD_DIM = 128
SIDE = 64
MID = 4
FAR = 16
MESH = pl.DeviceIdType.MESH
F32 = jnp.float32
BF16 = jnp.bfloat16
SCALE = HEAD_DIM ** -0.5 * math.log2(math.e)


def nt(a, b):
    return lax.dot_general(a, b, (((1,), (1,)), ((), ())), preferred_element_type=F32)


def nn(a, b):
    return lax.dot_general(a, b, (((1,), (0,)), ((), ())), preferred_element_type=F32)


def iota(shape, dim):
    return lax.broadcasted_iota(jnp.int32, shape, dim)


def attend(q, k, v, allowed):
    s = jnp.where(allowed, nt(q, k) * SCALE, -jnp.inf)
    top = jnp.max(s, axis=-1, keepdims=True)
    raised = jnp.exp2(s - top)
    den = jnp.sum(raised, axis=-1, keepdims=True)
    return nn(raised.astype(BF16), v), top, den


def kernel(sp_n, heads, q_hbm, k_hbm, v_hbm, w_hbm, out_ref,
           q_in, k_in, v_in, w, pkv, kvf, near_lo, near_hi, ob, ret, att, att_other, acc_n, md_n,
           load_sem, kv_s, kv_r, q_s, q_r, up_s, up_r, dn_s, dn_r, near_s, near_r, ret_s, ret_r, tp_s, tp_r):
    rows = q_in.shape[0]
    chunk = rows // MID
    mm = rows // FAR
    e = HEAD_DIM
    p, c = lax.axis_index("sp"), lax.axis_index("tp")
    groups = sp_n // MID
    g, j = p // MID, p % MID

    loads = [
        pltpu.make_async_copy(src, dst, load_sem.at[n])
        for n, (src, dst) in enumerate(((k_hbm, k_in), (v_hbm, v_in), (q_hbm, q_in), (w_hbm, w)))
    ]
    for load in loads:
        load.start()

    barrier = pltpu.get_barrier_semaphore()

    def greet(sp, tp):
        pl.semaphore_signal(barrier, inc=1, device_id=(sp, tp), device_id_type=MESH)

    def mate(d):
        return g * MID + (j + d) % MID

    for d in range(1, MID):
        greet(mate(d), c)
    greet(p, 1 - c)
    has_dn, has_up = g > 0, g < groups - 1
    has_prev, has_next = p > 0, p < sp_n - 1

    @pl.when(has_dn)
    def _():
        greet(p - MID, c)

    @pl.when(has_up)
    def _():
        greet(p + MID, c)

    @pl.when(has_prev)
    def _():
        greet(p - 1, c)

    @pl.when(has_next)
    def _():
        greet(p + 1, c)

    def remote(src, dst, ss, rs, sp, tp):
        return pltpu.make_async_remote_copy(
            src_ref=src, dst_ref=dst, send_sem=ss, recv_sem=rs, device_id=(sp, tp), device_id_type=MESH)

    r, t = iota((rows, rows), 0), iota((rows, rows), 1)
    perm = (t == FAR * (r % mm) + MID * ((r % chunk) // mm) + r // chunk).astype(BF16)
    r, t = t, r
    back = (t == FAR * (r % mm) + MID * ((r % chunk) // mm) + r // chunk).astype(BF16)

    for n, x in enumerate((k_in, v_in, q_in)):
        loads[n].wait()
        moved = nn(perm, x[...]).astype(BF16)
        for h in range(heads):
            pkv[h, n] = moved[:, h * e:(h + 1) * e]

    def at(n, base=0):
        return pl.ds(pl.multiple_of(base + n * chunk, chunk), chunk)

    for h in range(heads):
        for n in range(3):
            kvf[h, n, at(j, rows), :] = pkv[h, n, at(j), :]

    def edge(test, rows_at):
        @pl.when(jnp.logical_not(test))
        def _():
            for h in range(heads):
                for n in range(2):
                    kvf[h, n, pl.ds(rows_at, rows), :] = jnp.zeros((rows, e), BF16)

    edge(has_dn, 0)
    edge(has_up, 2 * rows)

    @pl.when(jnp.logical_not(has_prev))
    def _():
        near_lo[...] = jnp.zeros_like(near_lo)

    @pl.when(jnp.logical_not(has_next))
    def _():
        near_hi[...] = jnp.zeros_like(near_hi)

    pl.semaphore_wait(
        barrier,
        MID + has_dn.astype(jnp.int32) + has_up.astype(jnp.int32)
        + has_prev.astype(jnp.int32) + has_next.astype(jnp.int32))

    def up(h, d):
        n = (j - d + MID) % MID
        src = pkv.at[h, 0:2, at(n), :] if d == 0 else kvf.at[h, 0:2, at(n, rows), :]
        return remote(src, kvf.at[h, 0:2, at(n), :], up_s.at[h, d], up_r.at[h, d], (p + MID) % sp_n, c)

    def down(h, d):
        n = (j - d + MID) % MID
        src = pkv.at[h, 0:2, at(n), :] if d == 0 else kvf.at[h, 0:2, at(n, rows), :]
        return remote(src, kvf.at[h, 0:2, at(n, 2 * rows), :], dn_s.at[h, d], dn_r.at[h, d], (p - MID + sp_n) % sp_n, c)

    def forward(h, d):
        @pl.when(has_up)
        def _():
            up(h, d).start()

        @pl.when(has_dn)
        def _():
            down(h, d).start()

    def kv(h, d, receive=False):
        dst = (j - d + MID) % MID if receive else j
        return remote(pkv.at[h, 0:2, at((j + d) % MID), :], kvf.at[h, 0:2, at(dst, rows), :],
                      kv_s.at[h, d - 1], kv_r.at[h, d - 1], mate(d), c)

    def queries(d, receive=False):
        dst = (j - d + MID) % MID if receive else j
        return remote(pkv.at[:, 2, at((j + d) % MID), :], kvf.at[:, 2, at(dst, rows), :],
                      q_s.at[d - 1], q_r.at[d - 1], mate(d), c)

    for h in range(heads):
        for d in range(1, MID):
            kv(h, d).start()
        forward(h, 0)
    for d in range(1, MID):
        queries(d).start()

    def near(n, to_next):
        src = (k_in, v_in)[n]
        if to_next:
            return remote(src.at[pl.ds(rows - SIDE, SIDE), :], near_lo.at[n],
                          near_s.at[n, 0], near_r.at[n, 0], (p + 1) % sp_n, c)
        return remote(src.at[pl.ds(0, SIDE), :], near_hi.at[n],
                      near_s.at[n, 1], near_r.at[n, 1], (p - 1 + sp_n) % sp_n, c)

    @pl.when(has_next)
    def _():
        for n in range(2):
            near(n, True).start()

    @pl.when(has_prev)
    def _():
        for n in range(2):
            near(n, False).start()

    for h in range(heads):
        for d in range(1, MID):
            kv(h, d, receive=True).wait_recv()
            forward(h, d)

    half = rows // 2
    span = half + 2 * SIDE
    qi, ki = iota((half, span), 0), iota((half, span), 1)

    def order(x):
        return chunk * (x // chunk) + (FAR // MID) * (x % mm) + (x % chunk) // mm

    dn_ok, up_ok = has_dn.astype(jnp.int32), has_up.astype(jnp.int32)
    gap = order(ki) - order(qi)
    band = (gap >= 0) & (gap <= 2 * SIDE)
    mid_ok = (band & ((ki >= SIDE) | (dn_ok == 1)), band & ((ki < span - SIDE) | (up_ok == 1)))
    far_span = 3 * chunk
    qi, ki = iota((chunk, far_span), 0), iota((chunk, far_span), 1)
    far_ok = ((ki >= qi) & (ki <= qi + 2 * SIDE) & ((ki >= chunk) | (dn_ok == 1))
              & ((ki < 2 * chunk) | (up_ok == 1)))
    lane = iota((rows, e), 1)
    for d in range(1, MID):
        queries(d, receive=True).wait_recv()
    pick = (iota((16, e), 0) == iota((16, e), 1)).astype(BF16)

    def result(h, d, receive=False):
        dst = (j - d + MID) % MID if receive else j
        return remote(ob.at[h, (j + d) % MID], ret.at[h, dst],
                      ret_s.at[h, d - 1], ret_r.at[h, d - 1], mate(d), c)

    for h in range(heads):
        @pl.when(has_dn)
        def _():
            for d in range(MID):
                up(h, d).wait_recv()

        @pl.when(has_up)
        def _():
            for d in range(MID):
                down(h, d).wait_recv()

        q = kvf[h, 2, pl.ds(rows, rows), :]
        kh, vh = kvf[h, 0], kvf[h, 1]
        mids = []
        for b in range(2):
            first = rows - chunk + b * half
            mids.append(attend(q[b * half:(b + 1) * half], kh[first:first + span], vh[first:first + span], mid_ok[b]))
        o1, t1, d1 = (jnp.concatenate([mids[0][n], mids[1][n]], axis=0) for n in range(3))
        q4 = q.reshape(MID, FAR // MID, mm, e)
        k4 = kh.reshape(3 * MID, FAR // MID, mm, e)
        v4 = vh.reshape(3 * MID, FAR // MID, mm, e)
        fars = [
            attend(q4[:, s].reshape(chunk, e), k4[:, s].reshape(far_span, e), v4[:, s].reshape(far_span, e), far_ok)
            for s in range(FAR // MID)
        ]
        o2, t2, d2 = (
            jnp.concatenate(
                [fars[s][n][i * mm:(i + 1) * mm] for i in range(MID) for s in range(FAR // MID)], axis=0)
            for n in range(3))
        top = jnp.maximum(t1, t2)
        e1, e2 = jnp.exp2(t1 - top), jnp.exp2(t2 - top)
        den = e1 * d1 + e2 * d2
        o = ((e1 * o1 + e2 * o2) / den).astype(BF16)
        log_den = jnp.broadcast_to(top + jnp.log2(den), (rows, e))
        one = log_den.astype(BF16).astype(F32)
        two = (log_den - one).astype(BF16).astype(F32)
        three = log_den - one - two
        parts = jnp.where(lane == 0, one, jnp.where(lane == 1, two, three)).astype(BF16)
        twice = [parts[i * chunk:(i + 1) * chunk] for i in range(MID) for _ in range(2)]
        flat = nt(pick, jnp.concatenate(twice, axis=0)).astype(BF16)
        for i in range(MID):
            ob[h, i, :chunk] = o[i * chunk:(i + 1) * chunk]
            ob[h, i, chunk:] = flat[:, 2 * i * chunk:2 * (i + 1) * chunk]
        for d in range(1, MID):
            result(h, d).start()
        ret[h, pl.ds(j, 1)] = ob[h, pl.ds(j, 1)]

    @pl.when(has_prev)
    def _():
        for n in range(2):
            near(n, True).wait_recv()

    @pl.when(has_next)
    def _():
        for n in range(2):
            near(n, False).wait_recv()

    qi, ki = iota((half, span), 0), iota((half, span), 1)
    band = (ki >= qi) & (ki <= qi + 2 * SIDE)
    lo_ok, hi_ok = has_prev.astype(jnp.int32), has_next.astype(jnp.int32)
    allowed = (band & ((ki >= SIDE) | (lo_ok == 1)), band & ((ki < span - SIDE) | (hi_ok == 1)))
    for h in range(heads):
        cols = slice(h * e, (h + 1) * e)
        ks = [jnp.concatenate([near_lo[n, :, cols], x[:, cols], near_hi[n, :, cols]], axis=0)
              for n, x in enumerate((k_in, v_in))]
        for b in range(2):
            at_b = slice(b * half, (b + 1) * half)
            o, top, den = attend(q_in[at_b, cols], ks[0][b * half:b * half + span],
                                 ks[1][b * half:b * half + span], allowed[b])
            acc_n[h, at_b, :] = o
            md_n[h, 0, at_b, :] = jnp.broadcast_to(top, (half, e))
            md_n[h, 1, at_b, :] = jnp.broadcast_to(den, (half, e))

    r, t = iota((rows, 2 * rows), 1), iota((rows, 2 * rows), 0)
    low = r % (2 * chunk) < chunk
    r = r // (2 * chunk) * chunk + r % (2 * chunk)
    back_twice = (low & (t == FAR * (r % mm) + MID * ((r % chunk) // mm) + r // chunk)).astype(BF16)

    def share(h):
        cols = pl.ds(h * e, e)
        return remote(att.at[:, cols], att_other.at[:, cols], tp_s.at[h], tp_r.at[h], p, 1 - c)

    for h in range(heads):
        for d in range(1, MID):
            result(h, d, receive=True).wait_recv()
        o = nn(back, jnp.concatenate([ret[h, i, :chunk] for i in range(MID)], axis=0))
        parts = nt(back_twice, jnp.concatenate([ret[h, i, chunk:] for i in range(MID)], axis=1))
        log_den = parts[:, 0:1] + parts[:, 1:2] + parts[:, 2:3]
        t_n, d_n = md_n[h, 0], md_n[h, 1]
        top = jnp.maximum(t_n, log_den)
        e1, e2 = jnp.exp2(t_n - top), jnp.exp2(log_den - top)
        att[:, h * e:(h + 1) * e] = ((e1 * acc_n[h] + e2 * o) / (e1 * d_n + e2)).astype(BF16)
        share(h).start()

    width = heads * e
    loads[3].wait()
    own = nn(att[...], w[pl.ds(pl.multiple_of(c * width, width), width), :])
    for h in range(heads):
        share(h).wait_recv()
    other = nn(att_other[...], w[pl.ds(pl.multiple_of((1 - c) * width, width), width), :])
    out_ref[...] = (own + other).astype(BF16)

    for h in range(heads):
        for d in range(1, MID):
            kv(h, d).wait_send()
            result(h, d).wait_send()
        share(h).wait_send()
    for d in range(1, MID):
        queries(d).wait_send()
    @pl.when(has_up)
    def _():
        for h in range(heads):
            for d in range(MID):
                up(h, d).wait_send()

    @pl.when(has_dn)
    def _():
        for h in range(heads):
            for d in range(MID):
                down(h, d).wait_send()

    @pl.when(has_next)
    def _():
        for n in range(2):
            near(n, True).wait_send()

    @pl.when(has_prev)
    def _():
        for n in range(2):
            near(n, False).wait_send()


def per_device(sp_n, q, k, v, w):
    rows, columns = q.shape
    heads = columns // HEAD_DIM
    assert MID * rows == SIDE * FAR and rows // MID == SIDE and sp_n % MID == 0
    dma = pltpu.SemaphoreType.DMA
    e, chunk = HEAD_DIM, rows // MID
    return pl.pallas_call(
        functools.partial(kernel, sp_n, heads),
        out_shape=jax.ShapeDtypeStruct((rows, w.shape[1]), BF16),
        in_specs=[pl.BlockSpec(memory_space=pl.ANY)] * 4,
        out_specs=pl.BlockSpec(memory_space=pltpu.VMEM),
        scratch_shapes=[
            pltpu.VMEM((rows, columns), BF16),
            pltpu.VMEM((rows, columns), BF16),
            pltpu.VMEM((rows, columns), BF16),
            pltpu.VMEM(w.shape, BF16),
            pltpu.VMEM((heads, 3, rows, e), BF16),
            pltpu.VMEM((heads, 3, 3 * rows, e), BF16),
            pltpu.VMEM((2, SIDE, columns), BF16),
            pltpu.VMEM((2, SIDE, columns), BF16),
            pltpu.VMEM((heads, MID, chunk + 16, e), BF16),
            pltpu.VMEM((heads, MID, chunk + 16, e), BF16),
            pltpu.VMEM((rows, columns), BF16),
            pltpu.VMEM((rows, columns), BF16),
            pltpu.VMEM((heads, rows, e), F32),
            pltpu.VMEM((heads, 2, rows, e), F32),
            dma((4,)),
            dma((heads, MID - 1)), dma((heads, MID - 1)),
            dma((MID - 1,)), dma((MID - 1,)),
            dma((heads, MID)), dma((heads, MID)),
            dma((heads, MID)), dma((heads, MID)),
            dma((2, 2)), dma((2, 2)),
            dma((heads, MID - 1)), dma((heads, MID - 1)),
            dma((heads,)), dma((heads,)),
        ],
        compiler_params=pltpu.CompilerParams(collective_id=0, has_side_effects=True),
    )(q, k, v, w)


def solution(mesh):
    return jax.shard_map(
        functools.partial(per_device, mesh.shape["sp"]), mesh=mesh,
        in_specs=(P("sp", "tp"), P("sp", "tp"), P("sp", "tp"), P(None, "tp")),
        out_specs=P("sp", "tp"), check_vma=False,
    )
```

```python
import functools
import math

import jax
import jax.numpy as jnp
from jax import lax
from jax.experimental import pallas as pl
from jax.experimental.pallas import tpu as pltpu
from jax.sharding import PartitionSpec as P

HEAD_DIM = 128
SIDE = 64
MID = 4
FAR = 16
MESH = pl.DeviceIdType.MESH
F32 = jnp.float32
BF16 = jnp.bfloat16
SCALE = HEAD_DIM ** -0.5 * math.log2(math.e)


def nt(a, b):
    return lax.dot_general(a, b, (((1,), (1,)), ((), ())), preferred_element_type=F32)


def nn(a, b):
    return lax.dot_general(a, b, (((1,), (0,)), ((), ())), preferred_element_type=F32)


def iota(shape, dim):
    return lax.broadcasted_iota(jnp.int32, shape, dim)


def attend(q, k, v, allowed):
    s = jnp.where(allowed, nt(q, k) * SCALE, -jnp.inf)
    top = jnp.max(s, axis=-1, keepdims=True)
    raised = jnp.exp2(s - top)
    den = jnp.sum(raised, axis=-1, keepdims=True)
    return nn(raised.astype(BF16), v), top, den


def kernel(sp_n, heads, q_hbm, k_hbm, v_hbm, out_ref,
           q_in, k_in, v_in, pkv, kvf, near_lo, near_hi, ob, ret, att, att_other, acc_n, md_n,
           load_sem, kv_s, kv_r, q_s, q_r, up_s, up_r, dn_s, dn_r, near_s, near_r, ret_s, ret_r, tp_s, tp_r):
    rows = q_in.shape[0]
    chunk = rows // MID
    mm = rows // FAR
    e = HEAD_DIM
    p, c = lax.axis_index("sp"), lax.axis_index("tp")
    groups = sp_n // MID
    g, j = p // MID, p % MID

    loads = [
        pltpu.make_async_copy(src, dst, load_sem.at[n])
        for n, (src, dst) in enumerate(((k_hbm, k_in), (v_hbm, v_in), (q_hbm, q_in)))
    ]
    for load in loads:
        load.start()

    barrier = pltpu.get_barrier_semaphore()

    def greet(sp, tp):
        pl.semaphore_signal(barrier, inc=1, device_id=(sp, tp), device_id_type=MESH)

    def mate(d):
        return g * MID + (j + d) % MID

    for d in range(1, MID):
        greet(mate(d), c)
    greet(p, 1 - c)
    has_dn, has_up = g > 0, g < groups - 1
    has_prev, has_next = p > 0, p < sp_n - 1

    @pl.when(has_dn)
    def _():
        greet(p - MID, c)

    @pl.when(has_up)
    def _():
        greet(p + MID, c)

    @pl.when(has_prev)
    def _():
        greet(p - 1, c)

    @pl.when(has_next)
    def _():
        greet(p + 1, c)

    def remote(src, dst, ss, rs, sp, tp):
        return pltpu.make_async_remote_copy(
            src_ref=src, dst_ref=dst, send_sem=ss, recv_sem=rs, device_id=(sp, tp), device_id_type=MESH)

    r, t = iota((rows, rows), 0), iota((rows, rows), 1)
    perm = (t == FAR * (r % mm) + MID * ((r % chunk) // mm) + r // chunk).astype(BF16)
    r, t = t, r
    back = (t == FAR * (r % mm) + MID * ((r % chunk) // mm) + r // chunk).astype(BF16)

    for n, x in enumerate((k_in, v_in, q_in)):
        loads[n].wait()
        moved = nn(perm, x[...]).astype(BF16)
        for h in range(heads):
            pkv[h, n] = moved[:, h * e:(h + 1) * e]

    def at(n, base=0):
        return pl.ds(pl.multiple_of(base + n * chunk, chunk), chunk)

    for h in range(heads):
        for n in range(3):
            kvf[h, n, at(j, rows), :] = pkv[h, n, at(j), :]

    def edge(test, rows_at):
        @pl.when(jnp.logical_not(test))
        def _():
            for h in range(heads):
                for n in range(2):
                    kvf[h, n, pl.ds(rows_at, rows), :] = jnp.zeros((rows, e), BF16)

    edge(has_dn, 0)
    edge(has_up, 2 * rows)

    @pl.when(jnp.logical_not(has_prev))
    def _():
        near_lo[...] = jnp.zeros_like(near_lo)

    @pl.when(jnp.logical_not(has_next))
    def _():
        near_hi[...] = jnp.zeros_like(near_hi)

    pl.semaphore_wait(
        barrier,
        MID + has_dn.astype(jnp.int32) + has_up.astype(jnp.int32)
        + has_prev.astype(jnp.int32) + has_next.astype(jnp.int32))

    def up(h, d):
        n = (j - d + MID) % MID
        src = pkv.at[h, 0:2, at(n), :] if d == 0 else kvf.at[h, 0:2, at(n, rows), :]
        return remote(src, kvf.at[h, 0:2, at(n), :], up_s.at[h, d], up_r.at[h, d], (p + MID) % sp_n, c)

    def down(h, d):
        n = (j - d + MID) % MID
        src = pkv.at[h, 0:2, at(n), :] if d == 0 else kvf.at[h, 0:2, at(n, rows), :]
        return remote(src, kvf.at[h, 0:2, at(n, 2 * rows), :], dn_s.at[h, d], dn_r.at[h, d], (p - MID + sp_n) % sp_n, c)

    def forward(h, d):
        @pl.when(has_up)
        def _():
            up(h, d).start()

        @pl.when(has_dn)
        def _():
            down(h, d).start()

    def kv(h, d, receive=False):
        dst = (j - d + MID) % MID if receive else j
        return remote(pkv.at[h, 0:2, at((j + d) % MID), :], kvf.at[h, 0:2, at(dst, rows), :],
                      kv_s.at[h, d - 1], kv_r.at[h, d - 1], mate(d), c)

    def queries(d, receive=False):
        dst = (j - d + MID) % MID if receive else j
        return remote(pkv.at[:, 2, at((j + d) % MID), :], kvf.at[:, 2, at(dst, rows), :],
                      q_s.at[d - 1], q_r.at[d - 1], mate(d), c)

    for h in range(heads):
        for d in range(1, MID):
            kv(h, d).start()
        forward(h, 0)
    for d in range(1, MID):
        queries(d).start()

    def near(n, to_next):
        src = (k_in, v_in)[n]
        if to_next:
            return remote(src.at[pl.ds(rows - SIDE, SIDE), :], near_lo.at[n],
                          near_s.at[n, 0], near_r.at[n, 0], (p + 1) % sp_n, c)
        return remote(src.at[pl.ds(0, SIDE), :], near_hi.at[n],
                      near_s.at[n, 1], near_r.at[n, 1], (p - 1 + sp_n) % sp_n, c)

    @pl.when(has_next)
    def _():
        for n in range(2):
            near(n, True).start()

    @pl.when(has_prev)
    def _():
        for n in range(2):
            near(n, False).start()

    half = rows // 2
    own_span = half + SIDE
    qi, ki = iota((half, own_span), 0), iota((half, own_span), 1)
    for b in range(2):
        at_q = slice(b * half, (b + 1) * half)
        at_k = slice(b * (half - SIDE), b * (half - SIDE) + own_span)
        gap = (ki + at_k.start) - (qi + at_q.start)
        near_ok = (gap >= -SIDE) & (gap <= SIDE)
        for h in range(heads):
            cols = slice(h * e, (h + 1) * e)
            o, top, den = attend(q_in[at_q, cols], k_in[at_k, cols], v_in[at_k, cols], near_ok)
            acc_n[h, at_q, :] = o
            md_n[h, 0, at_q, :] = jnp.broadcast_to(top, (half, e))
            md_n[h, 1, at_q, :] = jnp.broadcast_to(den, (half, e))

    for h in range(heads):
        for d in range(1, MID):
            kv(h, d, receive=True).wait_recv()
            forward(h, d)

    span = half + 2 * SIDE
    qi, ki = iota((half, span), 0), iota((half, span), 1)

    def order(x):
        return chunk * (x // chunk) + (FAR // MID) * (x % mm) + (x % chunk) // mm

    dn_ok, up_ok = has_dn.astype(jnp.int32), has_up.astype(jnp.int32)
    gap = order(ki) - order(qi)
    band = (gap >= 0) & (gap <= 2 * SIDE)
    mid_ok = (band & ((ki >= SIDE) | (dn_ok == 1)), band & ((ki < span - SIDE) | (up_ok == 1)))
    far_span, ns = 4 * chunk, FAR // MID
    ones = jnp.ones((far_span, e), BF16)
    qi, ki = iota((chunk, far_span), 0), iota((chunk, far_span), 1)
    far_ok = ((ki >= qi) & (ki <= qi + 2 * SIDE) & ((ki >= chunk) | (dn_ok == 1))
              & ((ki < 2 * chunk) | (up_ok == 1)))
    lane = iota((rows, e), 1)
    for d in range(1, MID):
        queries(d, receive=True).wait_recv()
    pick = (iota((16, e), 0) == iota((16, e), 1)).astype(BF16)

    def result(h, d, receive=False):
        dst = (j - d + MID) % MID if receive else j
        return remote(ob.at[h, (j + d) % MID], ret.at[h, dst],
                      ret_s.at[h, d - 1], ret_r.at[h, d - 1], mate(d), c)

    for h in range(heads):
        @pl.when(has_dn)
        def _():
            for d in range(MID):
                up(h, d).wait_recv()

        @pl.when(has_up)
        def _():
            for d in range(MID):
                down(h, d).wait_recv()

        q = kvf[h, 2, pl.ds(rows, rows), :]
        kh, vh = kvf[h, 0], kvf[h, 1]
        firsts = [rows - chunk + b * half for b in range(2)]
        s_mid = jnp.concatenate([
            jnp.where(mid_ok[b], nt(q[b * half:(b + 1) * half], kh[f:f + span]), -jnp.inf)
            for b, f in enumerate(firsts)], axis=0)
        q4 = q.reshape(MID, ns, mm, e)

        def classes(x):
            x4 = x.reshape(3 * MID, ns, mm, e)
            return [jnp.concatenate([x4[:, n], x4[:MID, n]], axis=0).reshape(far_span, e) for n in range(ns)]

        k_far, v_far = classes(kh), classes(vh)
        far = [jnp.where(far_ok, nt(q4[:, n].reshape(chunk, e), k_far[n]), -jnp.inf) for n in range(ns)]
        s_far = jnp.concatenate([far[n][i * mm:(i + 1) * mm] for i in range(MID) for n in range(ns)], axis=0)
        peak = functools.reduce(
            jnp.maximum, [x[:, i:i + e] for x in (s_mid, s_far) for i in range(0, x.shape[1], e)])
        top = jnp.max(peak, axis=-1, keepdims=True)
        r_mid = jnp.exp2((s_mid - top) * SCALE).astype(BF16)
        r_far = jnp.exp2((s_far - top) * SCALE).astype(BF16)
        total = jnp.concatenate([
            nn(r_mid[b * half:(b + 1) * half], jnp.concatenate([vh[f:f + span], ones], axis=1))
            for b, f in enumerate(firsts)], axis=0)
        far = [
            nn(jnp.concatenate([r_far[(i * ns + n) * mm:(i * ns + n + 1) * mm] for i in range(MID)], axis=0),
               jnp.concatenate([v_far[n], ones], axis=1))
            for n in range(ns)]
        total += jnp.concatenate([far[n][i * mm:(i + 1) * mm] for i in range(MID) for n in range(ns)], axis=0)
        den = total[:, e:]
        o = (total[:, :e] / den).astype(BF16)
        log_den = top * SCALE + jnp.log2(den)
        one = log_den.astype(BF16).astype(F32)
        two = (log_den - one).astype(BF16).astype(F32)
        three = log_den - one - two
        parts = jnp.where(lane == 0, one, jnp.where(lane == 1, two, three)).astype(BF16)
        twice = [parts[i * chunk:(i + 1) * chunk] for i in range(MID) for _ in range(2)]
        flat = nt(pick, jnp.concatenate(twice, axis=0)).astype(BF16)
        for i in range(MID):
            ob[h, i, :chunk] = o[i * chunk:(i + 1) * chunk]
            ob[h, i, chunk:] = flat[:, 2 * i * chunk:2 * (i + 1) * chunk]
        for d in range(1, MID):
            result(h, d).start()
        ret[h, pl.ds(j, 1)] = ob[h, pl.ds(j, 1)]

    @pl.when(has_prev)
    def _():
        for n in range(2):
            near(n, True).wait_recv()

    @pl.when(has_next)
    def _():
        for n in range(2):
            near(n, False).wait_recv()

    lo_ok, hi_ok = has_prev.astype(jnp.int32), has_next.astype(jnp.int32)
    qi, ki = iota((SIDE, SIDE), 0), iota((SIDE, SIDE), 1)
    corners = (
        (near_lo, slice(0, SIDE), (ki >= qi) & (lo_ok == 1)),
        (near_hi, slice(rows - SIDE, rows), (ki <= qi) & (hi_ok == 1)),
    )
    for h in range(heads):
        cols = slice(h * e, (h + 1) * e)
        for halo, at_q, ok in corners:
            s = jnp.where(ok, nt(q_in[at_q, cols], halo[0, :, cols]) * SCALE, -jnp.inf)
            old = md_n[h, 0, at_q, :]
            top = jnp.maximum(old, jnp.max(s, axis=-1, keepdims=True))
            fade = jnp.exp2(old - top)
            raised = jnp.exp2(s - top[:, :SIDE])
            acc_n[h, at_q, :] = fade * acc_n[h, at_q, :] + nn(raised.astype(BF16), halo[1, :, cols])
            md_n[h, 0, at_q, :] = top
            md_n[h, 1, at_q, :] = fade * md_n[h, 1, at_q, :] + jnp.sum(raised, axis=-1, keepdims=True)

    r, t = iota((rows, 2 * rows), 1), iota((rows, 2 * rows), 0)
    low = r % (2 * chunk) < chunk
    r = r // (2 * chunk) * chunk + r % (2 * chunk)
    back_twice = (low & (t == FAR * (r % mm) + MID * ((r % chunk) // mm) + r // chunk)).astype(BF16)

    def share(h):
        cols = pl.ds(h * e, e)
        return remote(att.at[:, cols], att_other.at[:, cols], tp_s.at[h], tp_r.at[h], p, 1 - c)

    for h in range(heads):
        for d in range(1, MID):
            result(h, d, receive=True).wait_recv()
        o = nn(back, jnp.concatenate([ret[h, i, :chunk] for i in range(MID)], axis=0))
        parts = nt(back_twice, jnp.concatenate([ret[h, i, chunk:] for i in range(MID)], axis=1))
        log_den = parts[:, 0:1] + parts[:, 1:2] + parts[:, 2:3]
        t_n, d_n = md_n[h, 0], md_n[h, 1]
        top = jnp.maximum(t_n, log_den)
        e1, e2 = jnp.exp2(t_n - top), jnp.exp2(log_den - top)
        att[:, h * e:(h + 1) * e] = ((e1 * acc_n[h] + e2 * o) / (e1 * d_n + e2)).astype(BF16)
        share(h).start()

    width = heads * e
    out_ref[:, pl.ds(pl.multiple_of(c * width, width), width)] = att[...]
    for h in range(heads):
        share(h).wait_recv()
        out_ref[:, pl.ds(pl.multiple_of((1 - c) * width + h * e, e), e)] = att_other[:, h * e:(h + 1) * e]

    for h in range(heads):
        for d in range(1, MID):
            kv(h, d).wait_send()
            result(h, d).wait_send()
        share(h).wait_send()
    for d in range(1, MID):
        queries(d).wait_send()
    @pl.when(has_up)
    def _():
        for h in range(heads):
            for d in range(MID):
                up(h, d).wait_send()

    @pl.when(has_dn)
    def _():
        for h in range(heads):
            for d in range(MID):
                down(h, d).wait_send()

    @pl.when(has_next)
    def _():
        for n in range(2):
            near(n, True).wait_send()

    @pl.when(has_prev)
    def _():
        for n in range(2):
            near(n, False).wait_send()


def per_device(sp_n, q, k, v, w):
    rows, columns = q.shape
    heads = columns // HEAD_DIM
    assert MID * rows == SIDE * FAR and rows // MID == SIDE and sp_n % MID == 0
    dma = pltpu.SemaphoreType.DMA
    e, chunk = HEAD_DIM, rows // MID
    attended = pl.pallas_call(
        functools.partial(kernel, sp_n, heads),
        out_shape=jax.ShapeDtypeStruct((rows, w.shape[0]), BF16),
        in_specs=[pl.BlockSpec(memory_space=pl.ANY)] * 3,
        out_specs=pl.BlockSpec(memory_space=pltpu.VMEM),
        scratch_shapes=[
            pltpu.VMEM((rows, columns), BF16),
            pltpu.VMEM((rows, columns), BF16),
            pltpu.VMEM((rows, columns), BF16),
            pltpu.VMEM((heads, 3, rows, e), BF16),
            pltpu.VMEM((heads, 3, 3 * rows, e), BF16),
            pltpu.VMEM((2, SIDE, columns), BF16),
            pltpu.VMEM((2, SIDE, columns), BF16),
            pltpu.VMEM((heads, MID, chunk + 16, e), BF16),
            pltpu.VMEM((heads, MID, chunk + 16, e), BF16),
            pltpu.VMEM((rows, columns), BF16),
            pltpu.VMEM((rows, columns), BF16),
            pltpu.VMEM((heads, rows, e), F32),
            pltpu.VMEM((heads, 2, rows, e), F32),
            dma((3,)),
            dma((heads, MID - 1)), dma((heads, MID - 1)),
            dma((MID - 1,)), dma((MID - 1,)),
            dma((heads, MID)), dma((heads, MID)),
            dma((heads, MID)), dma((heads, MID)),
            dma((2, 2)), dma((2, 2)),
            dma((heads, MID - 1)), dma((heads, MID - 1)),
            dma((heads,)), dma((heads,)),
        ],
        compiler_params=pltpu.CompilerParams(collective_id=0, has_side_effects=True),
    )(q, k, v)
    return nn(attended, w).astype(BF16)


def solution(mesh):
    return jax.shard_map(
        functools.partial(per_device, mesh.shape["sp"]), mesh=mesh,
        in_specs=(P("sp", "tp"), P("sp", "tp"), P("sp", "tp"), P(None, "tp")),
        out_specs=P("sp", "tp"), check_vma=False,
    )
```

```python
import functools
import math

import jax
import jax.numpy as jnp
from jax import lax
from jax.experimental import pallas as pl
from jax.experimental.pallas import tpu as pltpu
from jax.sharding import PartitionSpec as P

HEAD_DIM = 128
SIDE = 64
MID = 4
FAR = 16
MESH = pl.DeviceIdType.MESH
F32 = jnp.float32
BF16 = jnp.bfloat16
SCALE = HEAD_DIM ** -0.5 * math.log2(math.e)


def nt(a, b):
    return lax.dot_general(a, b, (((1,), (1,)), ((), ())), preferred_element_type=F32)


def nn(a, b):
    return lax.dot_general(a, b, (((1,), (0,)), ((), ())), preferred_element_type=F32)


def iota(shape, dim):
    return lax.broadcasted_iota(jnp.int32, shape, dim)


def attend(q, k, v, allowed):
    s = jnp.where(allowed, nt(q, k) * SCALE, -jnp.inf)
    top = jnp.max(s, axis=-1, keepdims=True)
    raised = jnp.exp2(s - top)
    den = jnp.sum(raised, axis=-1, keepdims=True)
    return nn(raised.astype(BF16), v), top, den


def kernel(sp_n, heads, q_hbm, k_hbm, v_hbm, out_ref,
           q_in, k_in, v_in, pkv, kvf, near_lo, near_hi, ob, ret, att, att_other, acc_n, md_n,
           relay, load_sem, hop_s, hop_r, kv_s, kv_r, q_s, q_r, up_s, up_r, dn_s, dn_r, near_s, near_r, ret_s, ret_r, tp_s, tp_r):
    rows = q_in.shape[0]
    chunk = rows // MID
    mm = rows // FAR
    e = HEAD_DIM
    p, c = lax.axis_index("sp"), lax.axis_index("tp")
    groups = sp_n // MID
    g, j = p // MID, p % MID

    loads = [
        pltpu.make_async_copy(src, dst, load_sem.at[n])
        for n, (src, dst) in enumerate(((k_hbm, k_in), (v_hbm, v_in), (q_hbm, q_in)))
    ]
    for load in loads:
        load.start()

    barrier = pltpu.get_barrier_semaphore()

    def greet(sp, tp):
        pl.semaphore_signal(barrier, inc=1, device_id=(sp, tp), device_id_type=MESH)

    def mate(d):
        return g * MID + (j + d) % MID

    for d in range(1, MID):
        greet(mate(d), c)
    greet(p, 1 - c)
    has_dn, has_up = g > 0, g < groups - 1
    has_prev, has_next = p > 0, p < sp_n - 1

    @pl.when(has_dn)
    def _():
        greet(p - MID, c)

    @pl.when(has_up)
    def _():
        greet(p + MID, c)

    @pl.when(has_prev)
    def _():
        greet(p - 1, c)

    @pl.when(has_next)
    def _():
        greet(p + 1, c)

    def remote(src, dst, ss, rs, sp, tp):
        return pltpu.make_async_remote_copy(
            src_ref=src, dst_ref=dst, send_sem=ss, recv_sem=rs, device_id=(sp, tp), device_id_type=MESH)

    r, t = iota((rows, rows), 0), iota((rows, rows), 1)
    perm = (t == FAR * (r % mm) + MID * ((r % chunk) // mm) + r // chunk).astype(BF16)
    r, t = t, r
    back = (t == FAR * (r % mm) + MID * ((r % chunk) // mm) + r // chunk).astype(BF16)

    for n, x in enumerate((k_in, v_in, q_in)):
        loads[n].wait()
        moved = nn(perm, x[...]).astype(BF16)
        for h in range(heads):
            pkv[h, n] = moved[:, h * e:(h + 1) * e]

    def at(n, base=0):
        return pl.ds(pl.multiple_of(base + n * chunk, chunk), chunk)

    for h in range(heads):
        for n in range(3):
            kvf[h, n, at(j, rows), :] = pkv[h, n, at(j), :]

    def edge(test, rows_at):
        @pl.when(jnp.logical_not(test))
        def _():
            for h in range(heads):
                for n in range(2):
                    kvf[h, n, pl.ds(rows_at, rows), :] = jnp.zeros((rows, e), BF16)

    edge(has_dn, 0)
    edge(has_up, 2 * rows)

    @pl.when(jnp.logical_not(has_prev))
    def _():
        near_lo[...] = jnp.zeros_like(near_lo)

    @pl.when(jnp.logical_not(has_next))
    def _():
        near_hi[...] = jnp.zeros_like(near_hi)

    pl.semaphore_wait(
        barrier,
        MID + has_dn.astype(jnp.int32) + has_up.astype(jnp.int32)
        + has_prev.astype(jnp.int32) + has_next.astype(jnp.int32))

    def up(h, d):
        n = (j - d + MID) % MID
        src = pkv.at[h, 0:2, at(n), :] if d == 0 else kvf.at[h, 0:2, at(n, rows), :]
        return remote(src, kvf.at[h, 0:2, at(n), :], up_s.at[h, d], up_r.at[h, d], (p + MID) % sp_n, c)

    def down(h, d):
        n = (j - d + MID) % MID
        src = pkv.at[h, 0:2, at(n), :] if d == 0 else kvf.at[h, 0:2, at(n, rows), :]
        return remote(src, kvf.at[h, 0:2, at(n, 2 * rows), :], dn_s.at[h, d], dn_r.at[h, d], (p - MID + sp_n) % sp_n, c)

    def forward(h, d):
        @pl.when(has_up)
        def _():
            up(h, d).start()

        @pl.when(has_dn)
        def _():
            down(h, d).start()

    def kv(h, d, receive=False):
        dst = (j - d + MID) % MID if receive else j
        return remote(pkv.at[h, 0:2, at((j + d) % MID), :], kvf.at[h, 0:2, at(dst, rows), :],
                      kv_s.at[h, d - 1], kv_r.at[h, d - 1], mate(d), c)

    def queries(d, receive=False):
        dst = (j - d + MID) % MID if receive else j
        return remote(pkv.at[:, 2, at((j + d) % MID), :], kvf.at[:, 2, at(dst, rows), :],
                      q_s.at[d - 1], q_r.at[d - 1], mate(d), c)

    for h in range(heads):
        for d in range(1, MID):
            kv(h, d).start()
        forward(h, 0)
    for d in range(1, MID):
        queries(d).start()

    def near(n, to_next):
        src = (k_in, v_in)[n]
        if to_next:
            return remote(src.at[pl.ds(rows - SIDE, SIDE), :], near_lo.at[n],
                          near_s.at[n, 0], near_r.at[n, 0], (p + 1) % sp_n, c)
        return remote(src.at[pl.ds(0, SIDE), :], near_hi.at[n],
                      near_s.at[n, 1], near_r.at[n, 1], (p - 1 + sp_n) % sp_n, c)

    def hop(side):
        first = (rows - SIDE, 0)[side]
        to = ((p + MID) % sp_n, (p - MID + sp_n) % sp_n)[side]
        return remote(v_in.at[pl.ds(first, SIDE), :], relay.at[side], near_s.at[1, side], hop_r.at[side], to, c)

    def pass_on(side):
        dst = (near_lo, near_hi)[side]
        return remote(relay.at[side], dst.at[1], hop_s.at[side], near_r.at[1, side], mate((1, MID - 1)[side]), c)

    @pl.when(has_next)
    def _():
        near(0, True).start()

    @pl.when(has_prev)
    def _():
        near(0, False).start()

    @pl.when(has_next & (j < MID - 1))
    def _():
        near(1, True).start()

    @pl.when(has_prev & (j > 0))
    def _():
        near(1, False).start()

    @pl.when(has_up & (j == MID - 1))
    def _():
        hop(0).start()

    @pl.when(has_dn & (j == 0))
    def _():
        hop(1).start()

    half = rows // 2
    own_span = half + SIDE
    qi, ki = iota((half, own_span), 0), iota((half, own_span), 1)
    for b in range(2):
        at_q = slice(b * half, (b + 1) * half)
        at_k = slice(b * (half - SIDE), b * (half - SIDE) + own_span)
        gap = (ki + at_k.start) - (qi + at_q.start)
        near_ok = (gap >= -SIDE) & (gap <= SIDE)
        for h in range(heads):
            cols = slice(h * e, (h + 1) * e)
            o, top, den = attend(q_in[at_q, cols], k_in[at_k, cols], v_in[at_k, cols], near_ok)
            acc_n[h, at_q, :] = o
            md_n[h, 0, at_q, :] = jnp.broadcast_to(top, (half, e))
            md_n[h, 1, at_q, :] = jnp.broadcast_to(den, (half, e))

    for h in range(heads):
        for d in range(1, MID):
            kv(h, d, receive=True).wait_recv()
            forward(h, d)

    relays = (has_dn & (j == MID - 1), has_up & (j == 0))
    for side in range(2):
        @pl.when(relays[side])
        def _():
            hop(side).wait_recv()
            pass_on(side).start()

    span = half + 2 * SIDE
    qi, ki = iota((half, span), 0), iota((half, span), 1)

    def order(x):
        return chunk * (x // chunk) + (FAR // MID) * (x % mm) + (x % chunk) // mm

    dn_ok, up_ok = has_dn.astype(jnp.int32), has_up.astype(jnp.int32)
    gap = order(ki) - order(qi)
    band = (gap >= 0) & (gap <= 2 * SIDE)
    mid_ok = (band & ((ki >= SIDE) | (dn_ok == 1)), band & ((ki < span - SIDE) | (up_ok == 1)))
    far_span, ns = 4 * chunk, FAR // MID
    ones = jnp.ones((far_span, e), BF16)
    qi, ki = iota((chunk, far_span), 0), iota((chunk, far_span), 1)
    far_ok = ((ki >= qi) & (ki <= qi + 2 * SIDE) & ((ki >= chunk) | (dn_ok == 1))
              & ((ki < 2 * chunk) | (up_ok == 1)))
    lane = iota((rows, e), 1)
    for d in range(1, MID):
        queries(d, receive=True).wait_recv()
    pick = (iota((16, e), 0) == iota((16, e), 1)).astype(BF16)

    def result(h, d, receive=False):
        dst = (j - d + MID) % MID if receive else j
        return remote(ob.at[h, (j + d) % MID], ret.at[h, dst],
                      ret_s.at[h, d - 1], ret_r.at[h, d - 1], mate(d), c)

    for h in range(heads):
        @pl.when(has_dn)
        def _():
            for d in range(MID):
                up(h, d).wait_recv()

        @pl.when(has_up)
        def _():
            for d in range(MID):
                down(h, d).wait_recv()

        q = kvf[h, 2, pl.ds(rows, rows), :]
        kh, vh = kvf[h, 0], kvf[h, 1]
        firsts = [rows - chunk + b * half for b in range(2)]
        s_mid = jnp.concatenate([
            jnp.where(mid_ok[b], nt(q[b * half:(b + 1) * half], kh[f:f + span]), -jnp.inf)
            for b, f in enumerate(firsts)], axis=0)
        q4 = q.reshape(MID, ns, mm, e)

        def classes(x):
            x4 = x.reshape(3 * MID, ns, mm, e)
            return [jnp.concatenate([x4[:, n], x4[:MID, n]], axis=0).reshape(far_span, e) for n in range(ns)]

        k_far, v_far = classes(kh), classes(vh)
        far = [jnp.where(far_ok, nt(q4[:, n].reshape(chunk, e), k_far[n]), -jnp.inf) for n in range(ns)]
        s_far = jnp.concatenate([far[n][i * mm:(i + 1) * mm] for i in range(MID) for n in range(ns)], axis=0)
        peak = functools.reduce(
            jnp.maximum, [x[:, i:i + e] for x in (s_mid, s_far) for i in range(0, x.shape[1], e)])
        top = jnp.max(peak, axis=-1, keepdims=True)
        r_mid = jnp.exp2((s_mid - top) * SCALE).astype(BF16)
        r_far = jnp.exp2((s_far - top) * SCALE).astype(BF16)
        total = jnp.concatenate([
            nn(r_mid[b * half:(b + 1) * half], jnp.concatenate([vh[f:f + span], ones], axis=1))
            for b, f in enumerate(firsts)], axis=0)
        far = [
            nn(jnp.concatenate([r_far[(i * ns + n) * mm:(i * ns + n + 1) * mm] for i in range(MID)], axis=0),
               jnp.concatenate([v_far[n], ones], axis=1))
            for n in range(ns)]
        total += jnp.concatenate([far[n][i * mm:(i + 1) * mm] for i in range(MID) for n in range(ns)], axis=0)
        den = total[:, e:]
        o = (total[:, :e] / den).astype(BF16)
        log_den = top * SCALE + jnp.log2(den)
        one = log_den.astype(BF16).astype(F32)
        two = (log_den - one).astype(BF16).astype(F32)
        three = log_den - one - two
        parts = jnp.where(lane == 0, one, jnp.where(lane == 1, two, three)).astype(BF16)
        twice = [parts[i * chunk:(i + 1) * chunk] for i in range(MID) for _ in range(2)]
        flat = nt(pick, jnp.concatenate(twice, axis=0)).astype(BF16)
        for i in range(MID):
            ob[h, i, :chunk] = o[i * chunk:(i + 1) * chunk]
            ob[h, i, chunk:] = flat[:, 2 * i * chunk:2 * (i + 1) * chunk]
        for d in range(1, MID):
            result(h, d).start()
        ret[h, pl.ds(j, 1)] = ob[h, pl.ds(j, 1)]

    @pl.when(has_prev)
    def _():
        for n in range(2):
            near(n, True).wait_recv()

    @pl.when(has_next)
    def _():
        for n in range(2):
            near(n, False).wait_recv()

    lo_ok, hi_ok = has_prev.astype(jnp.int32), has_next.astype(jnp.int32)
    qi, ki = iota((SIDE, SIDE), 0), iota((SIDE, SIDE), 1)
    corners = (
        (near_lo, slice(0, SIDE), (ki >= qi) & (lo_ok == 1)),
        (near_hi, slice(rows - SIDE, rows), (ki <= qi) & (hi_ok == 1)),
    )
    for h in range(heads):
        cols = slice(h * e, (h + 1) * e)
        for halo, at_q, ok in corners:
            s = jnp.where(ok, nt(q_in[at_q, cols], halo[0, :, cols]) * SCALE, -jnp.inf)
            old = md_n[h, 0, at_q, :]
            top = jnp.maximum(old, jnp.max(s, axis=-1, keepdims=True))
            fade = jnp.exp2(old - top)
            raised = jnp.exp2(s - top[:, :SIDE])
            acc_n[h, at_q, :] = fade * acc_n[h, at_q, :] + nn(raised.astype(BF16), halo[1, :, cols])
            md_n[h, 0, at_q, :] = top
            md_n[h, 1, at_q, :] = fade * md_n[h, 1, at_q, :] + jnp.sum(raised, axis=-1, keepdims=True)

    r, t = iota((rows, 2 * rows), 1), iota((rows, 2 * rows), 0)
    low = r % (2 * chunk) < chunk
    r = r // (2 * chunk) * chunk + r % (2 * chunk)
    back_twice = (low & (t == FAR * (r % mm) + MID * ((r % chunk) // mm) + r // chunk)).astype(BF16)

    def share(h):
        cols = pl.ds(h * e, e)
        return remote(att.at[:, cols], att_other.at[:, cols], tp_s.at[h], tp_r.at[h], p, 1 - c)

    for h in range(heads):
        for d in range(1, MID):
            result(h, d, receive=True).wait_recv()
        o = nn(back, jnp.concatenate([ret[h, i, :chunk] for i in range(MID)], axis=0))
        parts = nt(back_twice, jnp.concatenate([ret[h, i, chunk:] for i in range(MID)], axis=1))
        log_den = parts[:, 0:1] + parts[:, 1:2] + parts[:, 2:3]
        t_n, d_n = md_n[h, 0], md_n[h, 1]
        top = jnp.maximum(t_n, log_den)
        e1, e2 = jnp.exp2(t_n - top), jnp.exp2(log_den - top)
        att[:, h * e:(h + 1) * e] = ((e1 * acc_n[h] + e2 * o) / (e1 * d_n + e2)).astype(BF16)
        share(h).start()

    width = heads * e
    out_ref[:, pl.ds(pl.multiple_of(c * width, width), width)] = att[...]
    for h in range(heads):
        share(h).wait_recv()
        out_ref[:, pl.ds(pl.multiple_of((1 - c) * width + h * e, e), e)] = att_other[:, h * e:(h + 1) * e]

    for h in range(heads):
        for d in range(1, MID):
            kv(h, d).wait_send()
            result(h, d).wait_send()
        share(h).wait_send()
    for d in range(1, MID):
        queries(d).wait_send()
    for side in range(2):
        @pl.when(relays[side])
        def _():
            pass_on(side).wait_send()
    @pl.when(has_up)
    def _():
        for h in range(heads):
            for d in range(MID):
                up(h, d).wait_send()

    @pl.when(has_dn)
    def _():
        for h in range(heads):
            for d in range(MID):
                down(h, d).wait_send()

    @pl.when(has_next)
    def _():
        for n in range(2):
            near(n, True).wait_send()

    @pl.when(has_prev)
    def _():
        for n in range(2):
            near(n, False).wait_send()


def per_device(sp_n, q, k, v, w):
    rows, columns = q.shape
    heads = columns // HEAD_DIM
    assert MID * rows == SIDE * FAR and rows // MID == SIDE and sp_n % MID == 0
    dma = pltpu.SemaphoreType.DMA
    e, chunk = HEAD_DIM, rows // MID
    attended = pl.pallas_call(
        functools.partial(kernel, sp_n, heads),
        out_shape=jax.ShapeDtypeStruct((rows, w.shape[0]), BF16),
        in_specs=[pl.BlockSpec(memory_space=pl.ANY)] * 3,
        out_specs=pl.BlockSpec(memory_space=pltpu.VMEM),
        scratch_shapes=[
            pltpu.VMEM((rows, columns), BF16),
            pltpu.VMEM((rows, columns), BF16),
            pltpu.VMEM((rows, columns), BF16),
            pltpu.VMEM((heads, 3, rows, e), BF16),
            pltpu.VMEM((heads, 3, 3 * rows, e), BF16),
            pltpu.VMEM((2, SIDE, columns), BF16),
            pltpu.VMEM((2, SIDE, columns), BF16),
            pltpu.VMEM((heads, MID, chunk + 16, e), BF16),
            pltpu.VMEM((heads, MID, chunk + 16, e), BF16),
            pltpu.VMEM((rows, columns), BF16),
            pltpu.VMEM((rows, columns), BF16),
            pltpu.VMEM((heads, rows, e), F32),
            pltpu.VMEM((heads, 2, rows, e), F32),
            pltpu.VMEM((2, SIDE, columns), BF16),
            dma((3,)),
            dma((2,)), dma((2,)),
            dma((heads, MID - 1)), dma((heads, MID - 1)),
            dma((MID - 1,)), dma((MID - 1,)),
            dma((heads, MID)), dma((heads, MID)),
            dma((heads, MID)), dma((heads, MID)),
            dma((2, 2)), dma((2, 2)),
            dma((heads, MID - 1)), dma((heads, MID - 1)),
            dma((heads,)), dma((heads,)),
        ],
        compiler_params=pltpu.CompilerParams(collective_id=0, has_side_effects=True),
    )(q, k, v)
    return nn(attended, w).astype(BF16)


def solution(mesh):
    return jax.shard_map(
        functools.partial(per_device, mesh.shape["sp"]), mesh=mesh,
        in_specs=(P("sp", "tp"), P("sp", "tp"), P("sp", "tp"), P(None, "tp")),
        out_specs=P("sp", "tp"), check_vma=False,
    )
```
